32 devices in a mesh: grp: 2 (over y), sp: 4 (over z), tp: 4 (over x, core).
Axes of the slice: x: 2, y: 2, z: 4, core: 2. Of those that a mesh axis runs over, the one named last changes fastest.
Arguments:
- latent: bfloat16 [1024, 2048], P(('grp', 'sp', 'tp')), parts along dimension 0, may hold values from -6 to 6
- context: bfloat16 [512, 2048], P(('grp', 'sp')), parts along dimension 0, may hold values from -6 to 6
- condition: float32 [4096], P('grp'), parts along dimension 0, may hold values from -6 to 6
- ctx_condition: float32 [2048], replicated, may hold values from -6 to 6
- w_mod: bfloat16 [2048, 6144], P('sp', 'tp'), may hold values from -0.125 to 0.125
- w_recept: bfloat16 [2048, 1024], P('sp', 'tp'), may hold values from -0.125 to 0.125
- w_key: bfloat16 [2048, 1024], P('sp', 'tp'), may hold values from -0.125 to 0.125
- w_value: bfloat16 [2048, 1024], P('sp', 'tp'), may hold values from -0.125 to 0.125
- w_decay_down: bfloat16 [2048, 64], replicated, may hold values from -0.125 to 0.125
- w_decay_up: bfloat16 [64, 1024], P(None, 'tp'), may hold values from -0.75 to 0.75
- decay_base: float32 [1024], P('tp'), may hold values from -12 to -3.5
- decay_shift: float32 [1024, 16], P(('grp', 'sp'), 'tp'), parts along dimension 0, may hold values from -1 to 26
- w_rate_down: bfloat16 [2048, 64], replicated, may hold values from -0.125 to 0.125
- w_rate_up: bfloat16 [64, 1024], P(None, 'tp'), may hold values from -0.75 to 0.75
- rate_bias: float32 [1024], P('tp'), may hold values from -8 to -1
- w_out: bfloat16 [1024, 2048], P('tp'), may hold values from -0.1875 to 0.1875
Outputs:
- mixed: bfloat16 [1024, 2048], P(('grp', 'sp', 'tp')), parts along dimension 0
The draws below stay inside these ranges and needn't reach their ends.
There are 2 independent parts, one for each index of `grp`. The reference program is written for one: setup_inputs(seed, part) draws one part's arguments, and reference() takes and returns one part's arrays. A program takes and returns all parts, laid end to end along the dimension named above; an argument that names none is the same for every part. Nothing has to cross between parts.
All inputs are finite; a program needn't handle non-finite values.
Results may differ from the reference program's by a relative error of at most 0.011.
Values may be sent and summed in bfloat16 or wider, within the bound.
A program may use at most 64 MiB of HBM per device.

```python
import jax
import jax.numpy as jnp
from jax import lax

D = 2048
HEAD_TOTAL = 16
HEAD = 64
RANK = 64
TOKENS_PER_SHARD = 128
CTX = 256
MIX_WIDTH = 1024
SAMPLE_TOKENS = 512
N_TP = 4


def fast_heads(key):
    fast_flag = jax.random.randint(jax.random.fold_in(key, 101), (HEAD_TOTAL,), 0, 2)
    return fast_flag == 1


def draw_decay_base(key, part):
    fast_flag = fast_heads(key)
    chain_len = CTX + SAMPLE_TOKENS
    slow_level = jnp.log(0.5 / chain_len) + jax.random.uniform(jax.random.fold_in(key, 11), (HEAD_TOTAL,), jnp.float32, -0.3, 0.3)
    fast_level = jax.random.uniform(jax.random.fold_in(key, 13), (HEAD_TOTAL,), jnp.float32, -5.0, -4.2)
    head_level = jnp.where(fast_flag, fast_level, slow_level)
    jitter = jax.random.uniform(jax.random.fold_in(key, 17), (HEAD_TOTAL, HEAD), jnp.float32, -0.3, 0.3)
    return (head_level[:, None] + jitter).reshape(MIX_WIDTH).astype(jnp.float32)


def draw_rate_bias(key, part):
    fast_flag = fast_heads(key)
    chain_len = CTX + SAMPLE_TOKENS
    slow_rate = jnp.minimum(HEAD * jax.random.uniform(jax.random.fold_in(key, 23), (HEAD_TOTAL, HEAD), jnp.float32, 0.4, 1.6) / chain_len, 0.2)
    fast_rate = jax.random.uniform(jax.random.fold_in(key, 29), (HEAD_TOTAL, HEAD), jnp.float32, 0.05, 0.2)
    rate_level = jnp.where(fast_flag[:, None], fast_rate, slow_rate)
    return jnp.log(rate_level / (1.0 - rate_level)).reshape(MIX_WIDTH).astype(jnp.float32)


def draw_decay_shift(key, part):
    block_total = SAMPLE_TOKENS // TOKENS_PER_SHARD
    offset_values = jax.random.uniform(jax.random.fold_in(key, 31), (block_total, HEAD_TOTAL), jnp.float32, -0.7, 0.7)
    token_positions = jnp.arange(SAMPLE_TOKENS, dtype=jnp.int32)
    spike_position = jax.random.randint(jax.random.fold_in(key, 37), (2, HEAD_TOTAL), 0, SAMPLE_TOKENS)
    spike_strength = jax.random.uniform(jax.random.fold_in(key, 41), (2, HEAD_TOTAL), jnp.float32, 11.0, 12.5)
    match_flags = token_positions[:, None, None] == spike_position[None, :, :]
    spike_events = jnp.sum(jnp.where(match_flags, spike_strength[None, :, :], 0.0), axis=1)
    return (jnp.repeat(offset_values, TOKENS_PER_SHARD, axis=0) + spike_events).astype(jnp.float32)


def level_of(rng, extent, cuts, low, high):
    def one(position, parts):
        steps = jax.random.uniform(jax.random.fold_in(jax.random.fold_in(rng, 6), position), (parts,), jnp.float32, low / len(cuts), high / len(cuts))
        return jnp.repeat(jnp.exp(steps), extent[position] // parts).reshape((-1,) + (1,) * (len(extent) - position - 1))

    loudness = one(*cuts[0])
    for cut in cuts[1:]:
        loudness = loudness * one(*cut)
    return loudness


def normal_values(rng, extent, scale, reach, cuts=(), kind=jnp.bfloat16):
    values = jax.random.normal(rng, extent, jnp.float32) * scale
    if len(cuts) > 0:
        values = level_of(rng, extent, cuts, -0.22, 0.18) * values
    return jnp.clip(values, min=-reach, max=reach).astype(kind)


def setup_inputs(seed: int = 0, part: int = 0) -> dict:
    splits = jax.random.split(jax.random.key(seed), 17)
    part_splits = jax.random.split(jax.random.fold_in(splits[16], part), 17)
    return {
        "latent": normal_values(part_splits[0], (SAMPLE_TOKENS, D), 1.0, 6.0, ((0, 16),)),
        "context": normal_values(part_splits[1], (CTX, D), 1.0, 6.0, ((0, 4),)),
        "condition": normal_values(part_splits[2], (D,), 1.0, 6.0, (), jnp.float32),
        "ctx_condition": normal_values(splits[3], (D,), 1.0, 6.0, (), jnp.float32),
        "w_mod": normal_values(splits[4], (D, 3 * D), D ** -0.5, 0.125, ((0, 4), (1, 4))),
        "w_recept": normal_values(splits[5], (D, MIX_WIDTH), D ** -0.5, 0.125, ((0, 4), (1, 4))),
        "w_key": normal_values(splits[6], (D, MIX_WIDTH), D ** -0.5, 0.125, ((0, 4), (1, 4))),
        "w_value": normal_values(splits[7], (D, MIX_WIDTH), D ** -0.5, 0.125, ((0, 4), (1, 4))),
        "w_decay_down": normal_values(splits[8], (D, RANK), D ** -0.5, 0.125),
        "w_decay_up": normal_values(splits[9], (RANK, MIX_WIDTH), RANK ** -0.5, 0.75, ((1, 4),)),
        "decay_base": draw_decay_base(jax.random.fold_in(splits[16], 71), part),
        "decay_shift": draw_decay_shift(jax.random.fold_in(jax.random.fold_in(splits[16], part), 71), part),
        "w_rate_down": normal_values(splits[12], (D, RANK), D ** -0.5, 0.125),
        "w_rate_up": normal_values(splits[13], (RANK, MIX_WIDTH), RANK ** -0.5, 0.75, ((1, 4),)),
        "rate_bias": draw_rate_bias(jax.random.fold_in(splits[16], 71), part),
        "w_out": normal_values(splits[15], (MIX_WIDTH, D), MIX_WIDTH ** -0.5, 0.1875, ((0, 4),)),
    }


NORM_EPS = 1e-06
HEAD_EPS = 0.00064
DECAY_SCALE = 0.6065306597126334
EXACT_MODE = lax.Precision.HIGHEST

def rounded(matrix):
    return lax.optimization_barrier(matrix.astype(jnp.bfloat16)).astype(jnp.float32)

def modulate(row_block, shift_row, scale_row):
    values = row_block.astype(jnp.float32)
    normed = values * lax.rsqrt(lax.optimization_barrier(jnp.mean(values * values, axis=-1, keepdims=True)) + NORM_EPS)
    return (normed * (1.0 + scale_row) + shift_row).astype(jnp.bfloat16)

def gate_terms(hidden, w_decay_down, w_decay_up, decay_base, w_rate_down, w_rate_up, rate_bias):
    decay_low = jnp.dot(hidden, w_decay_down, preferred_element_type=jnp.float32)
    squashed = jnp.tanh(rounded(decay_low)).astype(jnp.bfloat16)
    pre_decay = decay_base + jnp.dot(squashed, w_decay_up, preferred_element_type=jnp.float32)
    rate_low = jnp.dot(hidden, w_rate_down, preferred_element_type=jnp.float32).astype(jnp.bfloat16)
    rate_gate = jax.nn.sigmoid(rate_bias + jnp.dot(rate_low, w_rate_up, preferred_element_type=jnp.float32))
    return (pre_decay, rate_gate)

def advance_memory(memory, key_row, value_row, log_decay, rate_row):
    kappa_row = key_row * lax.rsqrt(lax.optimization_barrier(jnp.sum(key_row * key_row, axis=-1, keepdims=True)) + NORM_EPS)
    beta_row = kappa_row * rate_row
    removed = jnp.einsum('hvc,hc->hv', memory, kappa_row, precision=EXACT_MODE)
    return memory * jnp.exp(log_decay)[:, None, :] - removed[:, :, None] * beta_row[:, None, :] + value_row[:, :, None] * key_row[:, None, :]

def advance_context(memory, token_row):
    key_row, value_row, log_decay, rate_row = token_row
    return (advance_memory(memory, key_row, value_row, log_decay, rate_row), None)

def advance_latent(memory, token_row):
    key_row, value_row, log_decay, rate_row, receive = token_row
    memory = advance_memory(memory, key_row, value_row, log_decay, rate_row)
    return (memory, jnp.einsum('hvc,hc->hv', memory, receive, precision=EXACT_MODE))

def reference(latent, context, condition, ctx_condition, w_mod, w_recept, w_key, w_value, w_decay_down, w_decay_up, decay_base, decay_shift, w_rate_down, w_rate_up, rate_bias, w_out):
    activated = jax.nn.silu(jnp.stack([condition, ctx_condition])).astype(jnp.bfloat16)
    modulation = jnp.dot(activated, w_mod, preferred_element_type=jnp.float32)
    hidden_lat = modulate(latent, modulation[0, :D], modulation[0, D:2 * D])
    hidden_ctx = modulate(context, modulation[1, :D], modulation[1, D:2 * D])

    def split_heads(matrix):
        return matrix.reshape(matrix.shape[0], HEAD_TOTAL, HEAD)

    def project_heads(hidden, weight):
        return split_heads(rounded(jnp.dot(hidden, weight, preferred_element_type=jnp.float32)))
    pre_lat, rate_lat = gate_terms(hidden_lat, w_decay_down, w_decay_up, decay_base, w_rate_down, w_rate_up, rate_bias)
    pre_ctx, rate_ctx = gate_terms(hidden_ctx, w_decay_down, w_decay_up, decay_base, w_rate_down, w_rate_up, rate_bias)
    decay_lat = -DECAY_SCALE * jax.nn.sigmoid(split_heads(pre_lat) + decay_shift[:, :, None])
    decay_ctx = -DECAY_SCALE * jax.nn.sigmoid(split_heads(pre_ctx))
    lat_tokens = (project_heads(hidden_lat, w_key), project_heads(hidden_lat, w_value), decay_lat, split_heads(rate_lat), project_heads(hidden_lat, w_recept))
    ctx_tokens = (project_heads(hidden_ctx, w_key), project_heads(hidden_ctx, w_value), decay_ctx, split_heads(rate_ctx))
    zero_state = jnp.zeros((HEAD_TOTAL, HEAD, HEAD), jnp.float32)
    ctx_forward, _ = lax.scan(advance_context, zero_state, ctx_tokens)
    ctx_backward, _ = lax.scan(advance_context, zero_state, ctx_tokens, reverse=True)
    _, forward = lax.scan(advance_latent, ctx_forward, lat_tokens)
    _, backward = lax.scan(advance_latent, ctx_backward, lat_tokens, reverse=True)
    mixed_heads = forward + backward
    centred = mixed_heads - lax.optimization_barrier(jnp.mean(mixed_heads, axis=-1, keepdims=True))
    normed = centred * lax.rsqrt(lax.optimization_barrier(jnp.mean(centred * centred, axis=-1, keepdims=True)) + HEAD_EPS)
    normed = normed.reshape(SAMPLE_TOKENS, MIX_WIDTH).astype(jnp.bfloat16)
    group_width = MIX_WIDTH // N_TP
    summed = jnp.zeros((SAMPLE_TOKENS, D), jnp.float32)
    for group_index in range(N_TP):
        low_col = group_index * group_width
        partial_value = jnp.dot(normed[:, low_col:low_col + group_width], w_out[low_col:low_col + group_width], preferred_element_type=jnp.float32)
        summed = summed + rounded(partial_value)
    branch = rounded(summed)
    return (latent.astype(jnp.float32) + modulation[0, 2 * D:] * branch).astype(jnp.bfloat16)
```

```python
import functools

import jax
import jax.numpy as jnp
from jax import lax
from jax.experimental import pallas as pl
from jax.experimental.pallas import tpu as pltpu
from jax.sharding import PartitionSpec as P

HEAD = 64
BLOCK = 64
NORM_EPS = 1e-06
HEAD_EPS = 0.00064
DECAY_SCALE = 0.6065306597126334
MESH = pl.DeviceIdType.MESH
F32, BF16 = jnp.float32, jnp.bfloat16
NN = (((1,), (0,)), ((), ()))
NT = (((1,), (1,)), ((), ()))
TN = (((0,), (0,)), ((), ()))


def iota(shape, axis):
    return lax.broadcasted_iota(jnp.int32, shape, axis)


def mm(a, b, dims=NN):
    return lax.dot_general(a, b, dims, preferred_element_type=F32)


def split(x):
    high = x.astype(BF16)
    return (high, (x - high.astype(F32)).astype(BF16))


def mm3(a, b, dims=NN):
    return mm(a[0], b[0], dims) + (mm(a[1], b[0], dims) + mm(a[0], b[1], dims))


def mm2(a, b, dims=NN):
    return mm(a[0], b, dims) + mm(a[1], b, dims)


def block_diag(x, wide):
    rows, cols = x.shape
    heads = cols // wide
    shape = (heads * rows, cols)
    mask = (iota(shape, 0) // rows == iota(shape, 1) // wide).astype(F32)
    if rows % 16 == 0:
        return jnp.concatenate([x] * heads, axis=0) * mask.astype(x.dtype)
    return (jnp.concatenate([x.astype(F32)] * heads, axis=0) * mask).astype(x.dtype)


def bd(pair, wide):
    return (block_diag(pair[0], wide), block_diag(pair[1], wide))


def fold(full):
    size = full.shape[0]
    heads = size // HEAD
    kept = jnp.where(iota(full.shape, 0) // HEAD == iota(full.shape, 1) // HEAD, full, 0.0)
    total = kept[:HEAD]
    for h in range(1, heads):
        total = total + kept[h * HEAD : (h + 1) * HEAD]
    return total


def head_sum(x):
    size = x.shape[1]
    ones = (iota((size, size), 0) // HEAD == iota((size, size), 1) // HEAD).astype(F32).astype(BF16)
    return mm2(split(x), ones)


def block_map(key, value, log_decay, beta, kappa, receive, reverse):
    length, cols = key.shape
    heads = cols // HEAD
    row, col = iota((length, length), 0), iota((length, length), 1)
    reach = (col >= row) if reverse else (col <= row)
    reach = reach.astype(F32).astype(BF16)
    parts = split(log_decay)
    cumulative = mm(reach, parts[0]) + mm(reach, parts[1])
    previous = cumulative - log_decay
    mid = length // 2 if reverse else length // 2 - 1
    end = 0 if reverse else length - 1
    centre = cumulative[mid : mid + 1]
    closing = cumulative[end : end + 1]
    inward = jnp.exp(centre - cumulative)
    remain = jnp.exp(closing - cumulative)
    outward = kappa * jnp.exp(previous - centre)
    lhs = outward
    if receive is not None:
        lhs = jnp.concatenate([outward, receive * jnp.exp(cumulative - centre)], axis=0)
    lhs = split(lhs)
    mix_beta = mm3(lhs, bd(split(beta * inward), HEAD), NT)
    mix_key = mm3(lhs, bd(split(key * inward), HEAD), NT)
    shape = (length, heads * length)
    token, source = iota(shape, 0), iota(shape, 1) % length
    strict = (source > token) if reverse else (source < token)
    within = (source >= token) if reverse else (source <= token)
    strictly = jnp.where(strict, mix_beta[:length], 0.0)
    key_mix = jnp.where(strict, mix_key[:length], 0.0)
    eye = (source == token).astype(F32)
    inverse = eye - strictly
    parts = split(strictly)
    square = mm3(parts, bd(parts, length))
    rounds = (length - 1).bit_length() - 1
    for i in range(rounds):
        parts = split(square)
        rhs = bd(parts, length)
        if i == rounds - 1:
            inverse = inverse + mm3(split(inverse), rhs)
        else:
            both = mm3(split(jnp.concatenate([inverse, square], axis=0)), rhs)
            inverse = inverse + both[:length]
            square = both[length:]
    value_bf = value.astype(BF16)
    value_bd = block_diag(value_bf, HEAD)
    pushed = mm2(split(key_mix), value_bd)
    inverse = split(inverse)
    taken = mm3(inverse, bd(split(kappa * jnp.exp(previous)), HEAD))
    removed = mm3(inverse, bd(split(pushed), HEAD))
    beta_rest = split(beta * remain)
    size = (HEAD, cols)
    eye_row = iota(size, 0) == iota(size, 1) % HEAD
    move = jnp.where(eye_row, jnp.exp(closing), 0.0) - fold(mm3(split(taken), beta_rest, TN))
    key_rest = split(key * remain)
    write = mm(value_bf, key_rest[0], TN) + mm(value_bf, key_rest[1], TN)
    write = fold(write - mm3(split(removed), beta_rest, TN))
    if receive is None:
        return (move, write, None, None)
    read_key = split(jnp.where(within, mix_key[length:], 0.0))
    read_beta = split(jnp.where(within, mix_beta[length:], 0.0))
    query = receive * jnp.exp(cumulative) - mm3(read_beta, bd(split(taken), HEAD))
    local = mm2(read_key, value_bd) - mm3(read_beta, bd(split(removed), HEAD))
    return (move, write, query, local)


def step_state(state, move, write):
    return mm2(split(state), block_diag(move.astype(BF16), HEAD)) + write.astype(F32)


def chain_map(first, then):
    return (
        mm3(split(first[0]), bd(split(then[0]), HEAD)),
        mm3(split(first[1]), bd(split(then[0]), HEAD)) + then[1],
    )


def kernel(
    n_sp, n_tp,
    lat_ref, ctx_ref, cond_ref, ctx_cond_ref, w_mod_ref, w_recept_ref, w_key_ref, w_value_ref,
    decay_down_ref, decay_up_ref, decay_base_ref, decay_shift_ref, rate_down_ref, rate_up_ref,
    rate_bias_ref, w_out_ref,
    out_ref,
    mod_parts, mod_sum, mod_full, lat_all, hid, weights, acc, ctx_maps, ctx_own, lat_maps, lat_own,
    state, branch_own, branch_in,
    load_sem, msend, mrecv, gsend, grecv, lsend, lrecv, wsend, wrecv, csend, crecv,
    ssend, srecv, bsend, brecv,
):
    sp, tp = lax.axis_index("sp"), lax.axis_index("tp")
    model = lat_ref.shape[1]
    rows = lat_ref.shape[0]
    slab = w_mod_ref.shape[0]
    mod_cols = w_mod_ref.shape[1]
    cols = w_recept_ref.shape[1]
    tokens = rows * n_tp
    half = slab // 2

    loads = [
        pltpu.make_async_copy(ref, weights.at[sp, i], load_sem.at[i])
        for i, ref in enumerate((w_recept_ref, w_key_ref, w_value_ref))
    ]
    for load in loads:
        load.start()

    barrier = pltpu.get_barrier_semaphore()
    for k in range(1, n_sp):
        pl.semaphore_signal(
            barrier, inc=1, device_id={"sp": lax.rem(sp + k, n_sp)}, device_id_type=MESH
        )
    for k in range(1, n_tp):
        pl.semaphore_signal(
            barrier, inc=1, device_id={"tp": lax.rem(tp + k, n_tp)}, device_id_type=MESH
        )

    here = pl.ds(sp, 1)

    def silu(v):
        return v / (1.0 + jnp.exp(-v))

    activated = jnp.concatenate(
        [silu(cond_ref[here, :]), silu(ctx_cond_ref[here, :])], axis=0
    ).astype(BF16)
    mod_parts[0] = mm(activated, w_mod_ref[...])
    pl.semaphore_wait(barrier, n_sp - 1 + n_tp - 1)

    def remote(src, dst, send, recv, axis, target):
        return pltpu.make_async_remote_copy(
            src_ref=src, dst_ref=dst, send_sem=send, recv_sem=recv,
            device_id={axis: target}, device_id_type=MESH,
        )

    sent = []
    mods = []
    for k in range(1, n_sp):
        copy = remote(
            mod_parts.at[0], mod_parts.at[k], msend.at[k], mrecv.at[k], "sp", lax.rem(sp + k, n_sp)
        )
        copy.start()
        mods.append(copy)
    lats = []
    mine = pl.ds(pl.multiple_of(tp * rows, rows), rows)
    for k in range(1, n_tp):
        copy = remote(
            lat_ref, lat_all.at[mine, :], lsend.at[k], lrecv.at[k], "tp", lax.rem(tp + k, n_tp)
        )
        copy.start()
        lats.append(copy)
    lat_all[mine, :] = lat_ref[...]
    for load in loads:
        load.wait()
    right, left = lax.rem(sp + 1, n_sp), lax.rem(sp + n_sp - 1, n_sp)
    far = n_sp // 2

    def hop(i, direction):
        back = 1 if direction == 0 else -1
        which = lax.rem(sp + n_sp - back * (i - 1), n_sp)
        part = weights.at[which]
        if i == far:
            part = part.at[:, pl.ds(direction * half, half), :]
        return remote(
            part, part, wsend.at[direction, i], wrecv.at[direction, i], "sp",
            right if direction == 0 else left,
        )

    hops = {}
    for direction in range(2):
        hops[1, direction] = hop(1, direction)
        hops[1, direction].start()

    for copy in mods:
        copy.wait_recv()
    total = mod_parts[0]
    for k in range(1, n_sp):
        total = total + mod_parts[k]
    mod_sum[...] = total
    where_cols = pl.ds(pl.multiple_of(tp * mod_cols, mod_cols), mod_cols)
    mod_full[:, where_cols] = total
    gathers = []
    for k in range(1, n_tp):
        copy = remote(
            mod_sum, mod_full.at[:, where_cols], gsend.at[k], grecv.at[k], "tp",
            lax.rem(tp + k, n_tp),
        )
        copy.start()
        gathers.append(copy)
    for copy in lats:
        copy.wait_recv()
    for copy in gathers:
        copy.wait_recv()
    modulation = mod_full[...]

    def modulate(block, r):
        values = block.astype(F32)
        normed = values * lax.rsqrt(jnp.mean(values * values, axis=-1, keepdims=True) + NORM_EPS)
        return (
            normed * (1.0 + modulation[r : r + 1, model : 2 * model])
            + modulation[r : r + 1, :model]
        ).astype(BF16)

    hid[:tokens, :] = modulate(lat_all[...], 0)
    hid[tokens:, :] = modulate(ctx_ref[...], 1)
    hidden = hid[...]
    decay_low = jnp.tanh(mm(hidden, decay_down_ref[...]).astype(BF16).astype(F32)).astype(BF16)
    rate_low = mm(hidden, rate_down_ref[...]).astype(BF16)
    pre = decay_base_ref[...] + mm(decay_low, decay_up_ref[...])
    rate = 1.0 / (1.0 + jnp.exp(-(rate_bias_ref[...] + mm(rate_low, rate_up_ref[...]))))

    def add_slab(which, first=False):
        lanes = pl.ds(pl.multiple_of(which * slab, slab), slab) if slab % 128 == 0 else None
        if lanes is None:
            return
        piece = hid[:, lanes]
        for m in range(3):
            product = mm(piece, weights[which, m])
            acc[m] = product if first else acc[m] + product

    by_slab = slab % 128 == 0
    if by_slab:
        add_slab(sp, True)
    for i in range(1, far + 1):
        for direction in range(2):
            hops[i, direction].wait_recv()
        if i < far:
            for direction in range(2):
                hops[i + 1, direction] = hop(i + 1, direction)
                hops[i + 1, direction].start()
        if by_slab:
            add_slab(lax.rem(sp + n_sp - i, n_sp))
            if i < far:
                add_slab(lax.rem(sp + i, n_sp))
    if not by_slab:
        for m in range(3):
            joined = jnp.concatenate([weights[j, m] for j in range(n_sp)], axis=0)
            acc[m] = mm(hidden, joined)

    receive = acc[0].astype(BF16).astype(F32)
    key = acc[1].astype(BF16).astype(F32)
    value = acc[2].astype(BF16).astype(F32)
    kappa = key * lax.rsqrt(head_sum(key * key) + NORM_EPS)
    beta = kappa * rate
    lane_head = iota((tokens, cols), 1) // HEAD
    shift = jnp.zeros((tokens, cols), F32)
    for h in range(cols // HEAD):
        shift = jnp.where(lane_head == h, decay_shift_ref[:, h : h + 1], shift)
    pre = jnp.concatenate([pre[:tokens] + shift, pre[tokens:]], axis=0)
    log_decay = -DECAY_SCALE / (1.0 + jnp.exp(-pre))

    def blocks(start, stop, reverse, with_read):
        found = []
        length = min(BLOCK, stop - start)
        for low in range(start, stop, length):
            at = slice(low, low + length)
            found.append(
                block_map(
                    key[at], value[at], log_decay[at], beta[at], kappa[at],
                    receive[at] if with_read else None, reverse,
                )
            )
        return found

    def joined(found, reverse):
        order = found[::-1] if reverse else found
        result = (order[0][0], order[0][1])
        for one in order[1:]:
            result = chain_map(result, (one[0], one[1]))
        return result

    ctx_end = hid.shape[0]
    for d in range(2):
        move, write = joined(blocks(tokens, ctx_end, d == 1, False), d == 1)
        ctx_own[d, :HEAD] = move.astype(BF16)
        ctx_own[d, HEAD:] = write.astype(BF16)
    ctxs = []
    for k in range(1, n_sp):
        copy = remote(
            ctx_own, ctx_maps.at[sp], csend.at[k], crecv.at[k], "sp", lax.rem(sp + k, n_sp)
        )
        copy.start()
        ctxs.append(copy)
    ctx_maps[sp] = ctx_own[...]

    founds = []
    for d in range(2):
        found = blocks(0, tokens, d == 1, True)
        founds.append(found)
        move, write = joined(found, d == 1)
        lat_own[d, :HEAD] = move.astype(BF16)
        lat_own[d, HEAD:] = write.astype(BF16)

    def lat_copy(k, d):
        target = sp + k if d == 0 else sp - k
        return remote(
            lat_own.at[d], lat_maps.at[d, sp], ssend.at[d, k], srecv.at[d, k], "sp", target
        )

    for k in range(1, n_sp):

        @pl.when(sp + k < n_sp)
        def _():
            lat_copy(k, 0).start()

        @pl.when(sp - k >= 0)
        def _():
            lat_copy(k, 1).start()

    for copy in ctxs:
        copy.wait_recv()
    fwd = ctx_maps[0, 0, HEAD:].astype(F32)
    bwd = ctx_maps[n_sp - 1, 1, HEAD:].astype(F32)
    for j in range(1, n_sp):
        fwd = step_state(fwd, ctx_maps[j, 0, :HEAD], ctx_maps[j, 0, HEAD:])
        at = n_sp - 1 - j
        bwd = step_state(bwd, ctx_maps[at, 1, :HEAD], ctx_maps[at, 1, HEAD:])
    state[0] = fwd
    state[1] = bwd
    for k in range(n_sp - 1, 0, -1):

        @pl.when(sp - k >= 0)
        def _():
            remote(
                lat_own.at[0], lat_maps.at[0, sp - k], ssend.at[0, k], srecv.at[0, k], "sp", sp - k
            ).wait_recv()
            state[0] = step_state(
                state[0], lat_maps[0, sp - k, :HEAD], lat_maps[0, sp - k, HEAD:]
            )

        @pl.when(sp + k < n_sp)
        def _():
            remote(
                lat_own.at[1], lat_maps.at[1, sp + k], ssend.at[1, k], srecv.at[1, k], "sp", sp + k
            ).wait_recv()
            state[1] = step_state(
                state[1], lat_maps[1, sp + k, :HEAD], lat_maps[1, sp + k, HEAD:]
            )

    outputs = []
    for d in range(2):
        entering = state[d]
        found = founds[d]
        order = list(range(len(found)))
        if d == 1:
            order = order[::-1]
        got = [None] * len(found)
        for n, b in enumerate(order):
            move, write, query, local = found[b]
            got[b] = mm3(split(query), bd(split(entering), HEAD), NT) + local
            if n + 1 < len(order):
                entering = mm3(split(entering), bd(split(move), HEAD)) + write
        outputs.append(jnp.concatenate(got, axis=0))
    mixed = outputs[0] + outputs[1]
    centred = mixed - head_sum(mixed) * (1.0 / HEAD)
    variance = head_sum(centred * centred) * (1.0 / HEAD)
    normed = (centred * lax.rsqrt(variance + HEAD_EPS)).astype(BF16)
    product = mm(normed, w_out_ref[...]).astype(BF16)
    for t in range(n_tp):
        branch_own[t] = product[t * rows : (t + 1) * rows]
    backs = []
    for k in range(1, n_tp):
        target = lax.rem(tp + k, n_tp)
        copy = remote(
            branch_own.at[target], branch_in.at[k], bsend.at[k], brecv.at[k], "tp", target
        )
        copy.start()
        backs.append(copy)
    branch = branch_own[tp].astype(F32)
    for k, copy in enumerate(backs, 1):
        copy.wait_recv()
        branch = branch + branch_in[k].astype(F32)
    branch = branch.astype(BF16).astype(F32)
    gate = modulation[0:1, 2 * model :]
    out_ref[...] = (lat_ref[...].astype(F32) + gate * branch).astype(BF16)

    for copy in mods + lats + gathers + ctxs + backs + list(hops.values()):
        copy.wait_send()
    for k in range(1, n_sp):

        @pl.when(sp + k < n_sp)
        def _():
            lat_copy(k, 0).wait_send()

        @pl.when(sp - k >= 0)
        def _():
            lat_copy(k, 1).wait_send()


def shards(
    latent, context, condition, ctx_condition, w_mod, w_recept, w_key, w_value, w_decay_down,
    w_decay_up, decay_base, decay_shift, w_rate_down, w_rate_up, rate_bias, w_out,
):
    n_sp, n_tp = lax.axis_size("sp"), lax.axis_size("tp")
    rows, model = latent.shape
    slab, mod_cols = w_mod.shape
    cols = w_recept.shape[1]
    tokens = rows * n_tp
    every = tokens + context.shape[0]
    dma = pltpu.SemaphoreType.DMA
    vmem = pl.BlockSpec(memory_space=pltpu.VMEM)
    hbm = pl.BlockSpec(memory_space=pl.ANY)
    return pl.pallas_call(
        functools.partial(kernel, n_sp, n_tp),
        out_shape=jax.ShapeDtypeStruct((rows, model), BF16),
        in_specs=[vmem] * 5 + [hbm] * 3 + [vmem] * 8,
        out_specs=vmem,
        scratch_shapes=[
            pltpu.VMEM((n_sp, 2, mod_cols), F32),
            pltpu.VMEM((2, mod_cols), F32),
            pltpu.VMEM((2, mod_cols * n_tp), F32),
            pltpu.VMEM((tokens, model), BF16),
            pltpu.VMEM((every, model), BF16),
            pltpu.VMEM((n_sp, 3, slab, cols), BF16),
            pltpu.VMEM((3, every, cols), F32),
            pltpu.VMEM((n_sp, 2, 2 * HEAD, cols), BF16),
            pltpu.VMEM((2, 2 * HEAD, cols), BF16),
            pltpu.VMEM((2, n_sp, 2 * HEAD, cols), BF16),
            pltpu.VMEM((2, 2 * HEAD, cols), BF16),
            pltpu.VMEM((2, HEAD, cols), F32),
            pltpu.VMEM((n_tp, rows, model), BF16),
            pltpu.VMEM((n_tp, rows, model), BF16),
            dma((3,)),
            dma((n_sp,)), dma((n_sp,)),
            dma((n_tp,)), dma((n_tp,)),
            dma((n_tp,)), dma((n_tp,)),
            dma((2, n_sp // 2 + 1)), dma((2, n_sp // 2 + 1)),
            dma((n_sp,)), dma((n_sp,)),
            dma((2, n_sp)), dma((2, n_sp)),
            dma((n_tp,)), dma((n_tp,)),
        ],
        compiler_params=pltpu.CompilerParams(collective_id=0, has_side_effects=True),
    )(
        latent, context, condition.reshape(n_sp, slab),
        ctx_condition.reshape(n_sp, slab), w_mod, w_recept, w_key, w_value,
        w_decay_down, w_decay_up, decay_base[None], decay_shift, w_rate_down, w_rate_up,
        rate_bias[None], w_out,
    )


def solution(mesh):
    return jax.shard_map(
        shards,
        mesh=mesh,
        in_specs=(
            P(("grp", "sp", "tp"), None),
            P(("grp", "sp"), None),
            P("grp"),
            P(),
            P("sp", "tp"),
            P("sp", "tp"),
            P("sp", "tp"),
            P("sp", "tp"),
            P(),
            P(None, "tp"),
            P("tp"),
            P(("grp", "sp"), "tp"),
            P(),
            P(None, "tp"),
            P("tp"),
            P("tp", None),
        ),
        out_specs=P(("grp", "sp", "tp"), None),
        check_vma=False,
    )
```

```python
import functools

import jax
import jax.numpy as jnp
from jax import lax
from jax.experimental import pallas as pl
from jax.experimental.pallas import tpu as pltpu
from jax.sharding import PartitionSpec as P

HEAD = 64
BLOCK = 64
NORM_EPS = 1e-06
HEAD_EPS = 0.00064
DECAY_SCALE = 0.6065306597126334
MESH = pl.DeviceIdType.MESH
F32, BF16 = jnp.float32, jnp.bfloat16
NN = (((1,), (0,)), ((), ()))
NT = (((1,), (1,)), ((), ()))
TN = (((0,), (0,)), ((), ()))


def iota(shape, axis):
    return lax.broadcasted_iota(jnp.int32, shape, axis)


def mm(a, b, dims=NN):
    return lax.dot_general(a, b, dims, preferred_element_type=F32)


def split(x):
    high = x.astype(BF16)
    return (high, (x - high.astype(F32)).astype(BF16))


def mm3(a, b, dims=NN):
    return mm(a[0], b[0], dims) + (mm(a[1], b[0], dims) + mm(a[0], b[1], dims))


def mm2(a, b, dims=NN):
    return mm(a[0], b, dims) + mm(a[1], b, dims)


def block_diag(x, wide):
    rows, cols = x.shape
    heads = cols // wide
    shape = (heads * rows, cols)
    mask = (iota(shape, 0) // rows == iota(shape, 1) // wide).astype(F32)
    if rows % 16 == 0:
        return jnp.concatenate([x] * heads, axis=0) * mask.astype(x.dtype)
    return (jnp.concatenate([x.astype(F32)] * heads, axis=0) * mask).astype(x.dtype)


def bd(pair, wide):
    return (block_diag(pair[0], wide), block_diag(pair[1], wide))


def fold(full):
    size = full.shape[0]
    heads = size // HEAD
    kept = jnp.where(iota(full.shape, 0) // HEAD == iota(full.shape, 1) // HEAD, full, 0.0)
    total = kept[:HEAD]
    for h in range(1, heads):
        total = total + kept[h * HEAD : (h + 1) * HEAD]
    return total


def head_sum(x):
    size = x.shape[1]
    ones = (iota((size, size), 0) // HEAD == iota((size, size), 1) // HEAD).astype(F32).astype(BF16)
    return mm2(split(x), ones)


def lockstep(runs):
    results = [None] * len(runs)
    live = list(range(len(runs)))
    while live:
        still = []
        for i in live:
            try:
                next(runs[i])
                still.append(i)
            except StopIteration as end:
                results[i] = end.value
        live = still
    return results


def block_map(key, value, log_decay, beta, kappa, reverse):
    length, cols = key.shape
    heads = cols // HEAD
    row, col = iota((length, length), 0), iota((length, length), 1)
    reach = (col >= row) if reverse else (col <= row)
    reach = reach.astype(F32).astype(BF16)
    parts = split(log_decay)
    cumulative = mm(reach, parts[0]) + mm(reach, parts[1])
    yield
    previous = cumulative - log_decay
    mid = length // 2 if reverse else length // 2 - 1
    end = 0 if reverse else length - 1
    centre = cumulative[mid : mid + 1]
    closing = cumulative[end : end + 1]
    inward = jnp.exp(centre - cumulative)
    remain = jnp.exp(closing - cumulative)
    outward = split(kappa * jnp.exp(previous - centre))
    beta_in = bd(split(beta * inward), HEAD)
    key_in = bd(split(key * inward), HEAD)
    yield
    mix_beta = mm3(outward, beta_in, NT)
    mix_key = mm3(outward, key_in, NT)
    yield
    shape = (length, heads * length)
    token, source = iota(shape, 0), iota(shape, 1) % length
    strict = (source > token) if reverse else (source < token)
    within = (source >= token) if reverse else (source <= token)
    strictly = jnp.where(strict, mix_beta, 0.0)
    key_mix = jnp.where(strict, mix_key, 0.0)
    inverse = (source == token).astype(F32) - strictly
    parts = split(strictly)
    square = mm3(parts, bd(parts, length))
    value_bf = value.astype(BF16)
    value_bd = block_diag(value_bf, HEAD)
    pushed = mm2(split(key_mix), value_bd)
    yield
    rounds = (length - 1).bit_length() - 1
    for i in range(rounds):
        parts = split(square)
        rhs = bd(parts, length)
        if i == rounds - 1:
            inverse = inverse + mm3(split(inverse), rhs)
        else:
            both = mm3(split(jnp.concatenate([inverse, square], axis=0)), rhs)
            inverse = inverse + both[:length]
            square = both[length:]
        yield
    inverse = split(inverse)
    taken = mm3(inverse, bd(split(kappa * jnp.exp(previous)), HEAD))
    removed = mm3(inverse, bd(split(pushed), HEAD))
    yield
    taken, removed = split(taken), split(removed)
    beta_rest = split(beta * remain)
    key_rest = split(key * remain)
    size = (HEAD, cols)
    eye_row = iota(size, 0) == iota(size, 1) % HEAD
    move = jnp.where(eye_row, jnp.exp(closing), 0.0) - fold(mm3(taken, beta_rest, TN))
    write = mm(value_bf, key_rest[0], TN) + mm(value_bf, key_rest[1], TN)
    write = fold(write - mm3(removed, beta_rest, TN))
    return (move, write, (cumulative, centre, within, beta_in, key_in, value_bd, taken, removed))


def block_read(receive, kept):
    cumulative, centre, within, beta_in, key_in, value_bd, taken, removed = kept
    reading = split(receive * jnp.exp(cumulative - centre))
    read_beta = mm3(reading, beta_in, NT)
    read_key = mm3(reading, key_in, NT)
    yield
    read_key = split(jnp.where(within, read_key, 0.0))
    read_beta = split(jnp.where(within, read_beta, 0.0))
    query = receive * jnp.exp(cumulative) - mm3(read_beta, bd(taken, HEAD))
    local = mm2(read_key, value_bd) - mm3(read_beta, bd(removed, HEAD))
    return (query, local)


def step_state(state, move, write):
    return mm2(split(state), block_diag(move.astype(BF16), HEAD)) + write.astype(F32)


def chain_map(first, then):
    return (
        mm3(split(first[0]), bd(split(then[0]), HEAD)),
        mm3(split(first[1]), bd(split(then[0]), HEAD)) + then[1],
    )


def kernel(
    n_sp, n_tp,
    lat_ref, ctx_ref, cond_ref, ctx_cond_ref, w_mod_ref, w_recept_ref, w_key_ref, w_value_ref,
    decay_down_ref, decay_up_ref, decay_base_ref, decay_shift_ref, rate_down_ref, rate_up_ref,
    rate_bias_ref, w_out_ref,
    out_ref,
    mod_parts, mod_sum, mod_full, lat_all, hid, weights, ctx_maps, ctx_own, lat_maps, lat_own,
    state, branch_own, branch_in,
    load_sem, msend, mrecv, gsend, grecv, lsend, lrecv, wsend, wrecv, ysend, yrecv, csend, crecv,
    ssend, srecv, bsend, brecv,
):
    sp, tp = lax.axis_index("sp"), lax.axis_index("tp")
    model = lat_ref.shape[1]
    rows = lat_ref.shape[0]
    slab = w_mod_ref.shape[0]
    mod_cols = w_mod_ref.shape[1]
    cols = w_recept_ref.shape[1]
    tokens = rows * n_tp
    half = slab // 2

    grp = lax.axis_index("grp")
    loads = [
        pltpu.make_async_copy(
            ref,
            weights.at[m, pl.ds(pl.multiple_of(sp * slab, slab), slab), :],
            load_sem.at[m],
        )
        for m, ref in enumerate((w_key_ref, w_value_ref, w_recept_ref))
    ]
    for load in loads:
        load.start()

    barrier = pltpu.get_barrier_semaphore()
    for k in range(1, n_sp):
        pl.semaphore_signal(
            barrier, inc=1, device_id={"sp": lax.rem(sp + k, n_sp)}, device_id_type=MESH
        )
    for k in range(1, n_tp):
        pl.semaphore_signal(
            barrier, inc=1, device_id={"tp": lax.rem(tp + k, n_tp)}, device_id_type=MESH
        )

    pl.semaphore_signal(barrier, inc=1, device_id={"grp": 1 - grp}, device_id_type=MESH)

    if slab % 128 == 0:
        here = (slice(None), pl.ds(pl.multiple_of(sp * slab, slab), slab))
    else:
        here = (pl.ds(sp, 1), slice(None))

    def silu(v):
        return v / (1.0 + jnp.exp(-v))

    activated = jnp.concatenate(
        [silu(cond_ref[here]), silu(ctx_cond_ref[here])], axis=0
    ).astype(BF16)
    mod_parts[0] = mm(activated, w_mod_ref[...])
    pl.semaphore_wait(barrier, n_sp - 1 + n_tp - 1 + 1)

    def remote(src, dst, send, recv, axis, target):
        return pltpu.make_async_remote_copy(
            src_ref=src, dst_ref=dst, send_sem=send, recv_sem=recv,
            device_id={axis: target}, device_id_type=MESH,
        )

    sent = []
    mods = []
    for k in range(1, n_sp):
        copy = remote(
            mod_parts.at[0], mod_parts.at[k], msend.at[k], mrecv.at[k], "sp", lax.rem(sp + k, n_sp)
        )
        copy.start()
        mods.append(copy)
    lats = []
    mine = pl.ds(pl.multiple_of(tp * rows, rows), rows)
    for k in range(1, n_tp):
        copy = remote(
            lat_ref, lat_all.at[mine, :], lsend.at[k], lrecv.at[k], "tp", lax.rem(tp + k, n_tp)
        )
        copy.start()
        lats.append(copy)
    lat_all[mine, :] = lat_ref[...]
    for load in loads:
        load.wait()

    def piece(m, which, part):
        start = pl.multiple_of(which * slab + part * half, half)
        return weights.at[m, pl.ds(start, half), :]

    def hop(m, i, d):
        which = sp - (i - 1) if d == 0 else sp + (i - 1)
        part = piece(m, which, grp)
        return remote(
            part, part, wsend.at[m, d, i], wrecv.at[m, d, i], "sp", sp + 1 if d == 0 else sp - 1
        )

    def across(m, i, d):
        part = piece(m, sp - i if d == 0 else sp + i, grp)
        return remote(part, part, ysend.at[m, d, i], yrecv.at[m, d, i], "grp", 1 - grp)

    def crossed(m, i, d):
        part = piece(m, sp - i if d == 0 else sp + i, 1 - grp)
        return remote(part, part, ysend.at[m, d, i], yrecv.at[m, d, i], "grp", 1 - grp)

    def ahead(d):
        return sp + 1 < n_sp if d == 0 else sp >= 1

    def behind(i, d):
        return sp >= i if d == 0 else sp + i < n_sp

    for m in range(3):
        for d in range(2):
            pl.when(ahead(d))(lambda m=m, d=d: hop(m, 1, d).start())

    def relay(m, i):
        for d in range(2):

            @pl.when(behind(i, d))
            def _(d=d):
                came = piece(m, sp - i if d == 0 else sp + i, grp)
                remote(
                    came, came, wsend.at[m, d, i], wrecv.at[m, d, i], "sp",
                    sp + 1 if d == 0 else sp - 1,
                ).wait_recv()

                @pl.when(ahead(d))
                def _():
                    hop(m, i + 1, d).start()

                across(m, i, d).start()

    def relay_rest(m, first):
        def body(i, carry):
            relay(m, i)
            return carry

        lax.fori_loop(first, n_sp, body, 0)

    def arrive(m):
        def body(i, carry):
            for d in range(2):
                pl.when(behind(i, d))(lambda d=d: crossed(m, i, d).wait_recv())
            return carry

        lax.fori_loop(1, n_sp, body, 0)

    for copy in mods:
        copy.wait_recv()
    total = mod_parts[0]
    for k in range(1, n_sp):
        total = total + mod_parts[k]
    mod_sum[...] = total
    where_cols = pl.ds(pl.multiple_of(tp * mod_cols, mod_cols), mod_cols)
    mod_full[:, where_cols] = total
    gathers = []
    for k in range(1, n_tp):
        copy = remote(
            mod_sum, mod_full.at[:, where_cols], gsend.at[k], grecv.at[k], "tp",
            lax.rem(tp + k, n_tp),
        )
        copy.start()
        gathers.append(copy)
    relay(0, 1)
    for copy in lats:
        copy.wait_recv()
    for copy in gathers:
        copy.wait_recv()
    modulation = mod_full[...]

    def modulate(block, r):
        values = block.astype(F32)
        normed = values * lax.rsqrt(jnp.mean(values * values, axis=-1, keepdims=True) + NORM_EPS)
        return (
            normed * (1.0 + modulation[r : r + 1, model : 2 * model])
            + modulation[r : r + 1, :model]
        ).astype(BF16)

    hid[:tokens, :] = modulate(lat_all[...], 0)
    if n_sp > 2:
        relay(0, 2)
    hid[tokens:, :] = modulate(ctx_ref[...], 1)
    hidden = hid[...]
    decay_low = jnp.tanh(mm(hidden, decay_down_ref[...], NT).astype(BF16).astype(F32)).astype(BF16)
    rate_low = mm(hidden, rate_down_ref[...], NT).astype(BF16)
    pre = decay_base_ref[...] + mm(decay_low, decay_up_ref[...])
    rate = 1.0 / (1.0 + jnp.exp(-(rate_bias_ref[...] + mm(rate_low, rate_up_ref[...]))))

    relay_rest(0, 3)
    relay_rest(1, 1)
    arrive(0)
    key = mm(hidden, weights[0]).astype(BF16).astype(F32)
    relay_rest(2, 1)
    arrive(1)
    value = mm(hidden, weights[1]).astype(BF16).astype(F32)
    kappa = key * lax.rsqrt(head_sum(key * key) + NORM_EPS)
    beta = kappa * rate
    lane_head = iota((tokens, cols), 1) // HEAD
    shift = jnp.zeros((tokens, cols), F32)
    heads = cols // HEAD
    padded = jnp.concatenate(
        [decay_shift_ref[...], jnp.zeros(((-heads) % 8, tokens), F32)], axis=0
    )
    by_token = padded.T
    for h in range(heads):
        shift = jnp.where(lane_head == h, by_token[:, h : h + 1], shift)
    pre = jnp.concatenate([pre[:tokens] + shift, pre[tokens:]], axis=0)
    log_decay = -DECAY_SCALE / (1.0 + jnp.exp(-pre))

    def blocks(start, stop, reverse):
        length = min(BLOCK, stop - start)
        return [
            block_map(
                key[low : low + length], value[low : low + length],
                log_decay[low : low + length], beta[low : low + length],
                kappa[low : low + length], reverse,
            )
            for low in range(start, stop, length)
        ]

    def joined(found, reverse):
        order = found[::-1] if reverse else found
        result = (order[0][0], order[0][1])
        for one in order[1:]:
            result = chain_map(result, (one[0], one[1]))
        return result

    ctx_end = hid.shape[0]
    found = lockstep(blocks(tokens, ctx_end, False) + blocks(tokens, ctx_end, True))
    count = len(found) // 2
    for d in range(2):
        move, write = joined(found[d * count : (d + 1) * count], d == 1)
        ctx_own[d, :HEAD] = move.astype(BF16)
        ctx_own[d, HEAD:] = write.astype(BF16)
    ctxs = []
    for k in range(1, n_sp):
        copy = remote(
            ctx_own, ctx_maps.at[sp], csend.at[k], crecv.at[k], "sp", lax.rem(sp + k, n_sp)
        )
        copy.start()
        ctxs.append(copy)
    ctx_maps[sp] = ctx_own[...]

    found = lockstep(blocks(0, tokens, False) + blocks(0, tokens, True))
    count = len(found) // 2
    founds = [found[:count], found[count:]]
    for d in range(2):
        move, write = joined(founds[d], d == 1)
        lat_own[d, :HEAD] = move.astype(BF16)
        lat_own[d, HEAD:] = write.astype(BF16)

    def lat_copy(k, d):
        target = sp + k if d == 0 else sp - k
        return remote(
            lat_own.at[d], lat_maps.at[d, sp], ssend.at[d, k], srecv.at[d, k], "sp", target
        )

    for k in range(1, n_sp):

        @pl.when(sp + k < n_sp)
        def _():
            lat_copy(k, 0).start()

        @pl.when(sp - k >= 0)
        def _():
            lat_copy(k, 1).start()

    arrive(2)
    receive = mm(hidden[:tokens], weights[2]).astype(BF16).astype(F32)
    length = tokens // count
    reads = lockstep(
        [
            block_read(receive[b * length : (b + 1) * length], founds[d][b][2])
            for d in range(2)
            for b in range(count)
        ]
    )
    for copy in ctxs:
        copy.wait_recv()
    fwd = ctx_maps[0, 0, HEAD:].astype(F32)
    bwd = ctx_maps[n_sp - 1, 1, HEAD:].astype(F32)
    for j in range(1, n_sp):
        fwd = step_state(fwd, ctx_maps[j, 0, :HEAD], ctx_maps[j, 0, HEAD:])
        at = n_sp - 1 - j
        bwd = step_state(bwd, ctx_maps[at, 1, :HEAD], ctx_maps[at, 1, HEAD:])
    state[0] = fwd
    state[1] = bwd
    for k in range(n_sp - 1, 0, -1):

        @pl.when(sp - k >= 0)
        def _():
            remote(
                lat_own.at[0], lat_maps.at[0, sp - k], ssend.at[0, k], srecv.at[0, k], "sp", sp - k
            ).wait_recv()
            state[0] = step_state(
                state[0], lat_maps[0, sp - k, :HEAD], lat_maps[0, sp - k, HEAD:]
            )

        @pl.when(sp + k < n_sp)
        def _():
            remote(
                lat_own.at[1], lat_maps.at[1, sp + k], ssend.at[1, k], srecv.at[1, k], "sp", sp + k
            ).wait_recv()
            state[1] = step_state(
                state[1], lat_maps[1, sp + k, :HEAD], lat_maps[1, sp + k, HEAD:]
            )

    outputs = []
    for d in range(2):
        entering = state[d]
        found = founds[d]
        order = list(range(len(found)))
        if d == 1:
            order = order[::-1]
        got = [None] * len(found)
        for n, b in enumerate(order):
            move, write, _ = found[b]
            query, local = reads[d * count + b]
            got[b] = mm3(split(query), bd(split(entering), HEAD), NT) + local
            if n + 1 < len(order):
                entering = mm3(split(entering), bd(split(move), HEAD)) + write
        outputs.append(jnp.concatenate(got, axis=0))
    mixed = outputs[0] + outputs[1]
    centred = mixed - head_sum(mixed) * (1.0 / HEAD)
    variance = head_sum(centred * centred) * (1.0 / HEAD)
    normed = (centred * lax.rsqrt(variance + HEAD_EPS)).astype(BF16)
    product = mm(normed, w_out_ref[...]).astype(BF16)
    for t in range(n_tp):
        branch_own[t] = product[t * rows : (t + 1) * rows]
    backs = []
    for k in range(1, n_tp):
        target = lax.rem(tp + k, n_tp)
        copy = remote(
            branch_own.at[target], branch_in.at[k], bsend.at[k], brecv.at[k], "tp", target
        )
        copy.start()
        backs.append(copy)
    branch = branch_own[tp].astype(F32)
    for k, copy in enumerate(backs, 1):
        copy.wait_recv()
        branch = branch + branch_in[k].astype(F32)
    branch = branch.astype(BF16).astype(F32)
    gate = modulation[0:1, 2 * model :]
    out_ref[...] = (lat_ref[...].astype(F32) + gate * branch).astype(BF16)

    for copy in mods + lats + gathers + ctxs + backs:
        copy.wait_send()
    for k in range(1, n_sp):

        @pl.when(sp + k < n_sp)
        def _():
            lat_copy(k, 0).wait_send()

        @pl.when(sp - k >= 0)
        def _():
            lat_copy(k, 1).wait_send()

    def drain(i, carry):
        for m in range(3):
            for d in range(2):
                pl.when(behind(i - 1, d) & ahead(d))(lambda m=m, d=d: hop(m, i, d).wait_send())
                pl.when(behind(i, d))(lambda m=m, d=d: across(m, i, d).wait_send())
        return carry

    lax.fori_loop(1, n_sp, drain, 0)


def shards(
    latent, context, condition, ctx_condition, w_mod, w_recept, w_key, w_value, w_decay_down,
    w_decay_up, decay_base, decay_shift, w_rate_down, w_rate_up, rate_bias, w_out,
):
    n_sp, n_tp = lax.axis_size("sp"), lax.axis_size("tp")
    rows, model = latent.shape
    slab, mod_cols = w_mod.shape
    cols = w_recept.shape[1]
    tokens = rows * n_tp
    every = tokens + context.shape[0]
    by_row = (1, model) if slab % 128 == 0 else (n_sp, slab)
    dma = pltpu.SemaphoreType.DMA
    vmem = pl.BlockSpec(memory_space=pltpu.VMEM)
    hbm = pl.BlockSpec(memory_space=pl.ANY)
    return pl.pallas_call(
        functools.partial(kernel, n_sp, n_tp),
        out_shape=jax.ShapeDtypeStruct((rows, model), BF16),
        in_specs=[vmem] * 5 + [hbm] * 3 + [vmem] * 8,
        out_specs=vmem,
        scratch_shapes=[
            pltpu.VMEM((n_sp, 2, mod_cols), F32),
            pltpu.VMEM((2, mod_cols), F32),
            pltpu.VMEM((2, mod_cols * n_tp), F32),
            pltpu.VMEM((tokens, model), BF16),
            pltpu.VMEM((every, model), BF16),
            pltpu.VMEM((3, n_sp * slab, cols), BF16),
            pltpu.VMEM((n_sp, 2, 2 * HEAD, cols), BF16),
            pltpu.VMEM((2, 2 * HEAD, cols), BF16),
            pltpu.VMEM((2, n_sp, 2 * HEAD, cols), BF16),
            pltpu.VMEM((2, 2 * HEAD, cols), BF16),
            pltpu.VMEM((2, HEAD, cols), F32),
            pltpu.VMEM((n_tp, rows, model), BF16),
            pltpu.VMEM((n_tp, rows, model), BF16),
            dma((3,)),
            dma((n_sp,)), dma((n_sp,)),
            dma((n_tp,)), dma((n_tp,)),
            dma((n_tp,)), dma((n_tp,)),
            dma((3, 2, n_sp)), dma((3, 2, n_sp)), dma((3, 2, n_sp)), dma((3, 2, n_sp)),
            dma((n_sp,)), dma((n_sp,)),
            dma((2, n_sp)), dma((2, n_sp)),
            dma((n_tp,)), dma((n_tp,)),
        ],
        compiler_params=pltpu.CompilerParams(collective_id=0, has_side_effects=True),
    )(
        latent, context, condition.reshape(by_row),
        ctx_condition.reshape(by_row), w_mod, w_recept, w_key, w_value,
        w_decay_down.T, w_decay_up, decay_base[None], decay_shift.T, w_rate_down.T, w_rate_up,
        rate_bias[None], w_out,
    )


def solution(mesh):
    return jax.shard_map(
        shards,
        mesh=mesh,
        in_specs=(
            P(("grp", "sp", "tp"), None),
            P(("grp", "sp"), None),
            P("grp"),
            P(),
            P("sp", "tp"),
            P("sp", "tp"),
            P("sp", "tp"),
            P("sp", "tp"),
            P(),
            P(None, "tp"),
            P("tp"),
            P(("grp", "sp"), "tp"),
            P(),
            P(None, "tp"),
            P("tp"),
            P("tp", None),
        ),
        out_specs=P(("grp", "sp", "tp"), None),
        check_vma=False,
    )
```
